32 devices in a mesh: sp: 4 (over y, x), tp: 8 (over z, core).
Axes of the slice: x: 2, y: 2, z: 4, core: 2. Of those that a mesh axis runs over, the one named last changes fastest.
Arguments:
- residual_mid: bfloat16 [640, 4096], P('sp'), may hold values from -100 to 100
- out_grad: bfloat16 [640, 4096], P('sp'), may hold values from -6 to 6
- norm_gain: float32 [4096], replicated, may hold values from 0.1 to 1.9
- expert_ids: int32 [640, 2], P('sp'), may hold values from 0 to 3, all different within a row; in each aligned block of 160 rows (0 to 159, 160 to 319, ...) at most 160 rows name the same one
- expert_weights: float32 [640, 2], P('sp'), may hold values from 0.1 to 1
- gate_proj: bfloat16 [4, 4096, 2048], P('sp', None, 'tp'), may hold values from -0.25 to 0.25
- up_proj: bfloat16 [4, 4096, 2048], P('sp', None, 'tp'), may hold values from -0.25 to 0.25
- down_proj: bfloat16 [4, 2048, 4096], P('sp', 'tp'), may hold values from -0.125 to 0.125
- out_proj: bfloat16 [4096, 4096], P('tp'), may hold values from -0.09375 to 0.09375
- query_rows: bfloat16 [640, 4096], P('sp', 'tp'), may hold values from -6 to 6
- key_rows: bfloat16 [640, 4096], P('sp', 'tp'), may hold values from -6 to 6
- value_rows: bfloat16 [640, 4096], P('sp', 'tp'), may hold values from -6 to 6
- retention_out: bfloat16 [640, 4096], P('sp', 'tp'), may hold values from -6 to 6
- log_decay: float32 [640, 16], P('sp', 'tp'), may hold values from -2 to 0
- entry_state: float32 [4, 16, 256, 256], P('sp', 'tp'), may hold values from -24 to 24
Outputs:
- gate_grad: bfloat16 [4, 4096, 2048], P('sp', None, 'tp')
- up_grad: bfloat16 [4, 4096, 2048], P('sp', None, 'tp')
- down_grad: bfloat16 [4, 2048, 4096], P('sp', 'tp')
- proj_grad: float32 [4096, 4096], P('sp', 'tp')
- query_grad: bfloat16 [640, 4096], P('sp', 'tp')
- key_grad: bfloat16 [640, 4096], P('sp', 'tp')
- value_grad: bfloat16 [640, 4096], P('sp', 'tp')
The draws below stay inside these ranges and needn't reach their ends.
Inputs may be any that keep to these rules, and one draw needn't show every extreme that they name: `expert_ids`: each row names 2 different experts. Among the rows of one device, no expert is named by more than 160 rows, and in every draw some expert is named by exactly 160 rows of some device.
All inputs are finite; a program needn't handle non-finite values.
Results may differ from the reference program's by a relative error of at most 0.025.
The reference program's roundings to bfloat16 on the way count: a program that leaves them out, or rounds other values in their place, can miss the bound.
Values may be sent and summed in bfloat16 or wider, within the bound.
A program may use at most 128 MiB of HBM per device.

```python
import math
import jax
import jax.numpy as jnp
import numpy as np
from jax import lax

D = 4096
FF = 2048
RETENTION_HEADS = 16
DK = 256
TOP = 2
TOK_DEV = 160
RW = 4096
EXPERTS = 4
SEGS = 4
SEQUENCE_TOKENS = 640
CAP = 160
N_TP = 8


def draw_residual_mid(key, part):
    base_key, col_key, row_key = jax.random.split(key, 3)
    columns = jnp.exp(jax.random.uniform(col_key, (1, D), jnp.float32, 0.0, math.log(10.0)))
    rowscale = jnp.exp(jax.random.uniform(row_key, (SEQUENCE_TOKENS, 1), jnp.float32, math.log(0.3), math.log(3.0)))
    entries = jnp.clip(jax.random.normal(base_key, (SEQUENCE_TOKENS, D), jnp.float32), -6.0, 6.0)
    return (entries * columns * rowscale / 3.0).astype(jnp.bfloat16)


def draw_log_decay(key, part):
    random_keys = jax.random.split(key, 7)
    head_order = jax.random.permutation(random_keys[0], RETENTION_HEADS)
    fast_heads = head_order < RETENTION_HEADS // 2
    fast_span = jnp.exp(jax.random.uniform(random_keys[1], (RETENTION_HEADS,), jnp.float32, math.log(30.0), math.log(100.0)))
    slow_total = jax.random.uniform(random_keys[2], (RETENTION_HEADS,), jnp.float32, 0.05, 0.2) * math.log(10.0)
    decay_speed = jnp.where(fast_heads, math.log(20.0) / fast_span, slow_total / SEQUENCE_TOKENS)
    segment_multiplier = jnp.exp(jax.random.uniform(random_keys[3], (SEGS, RETENTION_HEADS), jnp.float32, math.log(0.5), math.log(2.0)))
    segment_multiplier = jnp.repeat(segment_multiplier, TOK_DEV, axis=0)
    jaggedness = jax.random.uniform(random_keys[4], (SEQUENCE_TOKENS, RETENTION_HEADS), jnp.float32, 0.5, 1.5)
    spike_position = jax.random.randint(random_keys[5], (2, 1), 0, SEQUENCE_TOKENS)
    spike_retained = jax.random.uniform(random_keys[6], (2, RETENTION_HEADS), jnp.float32, 0.5, 0.8)
    token_position = jnp.arange(SEQUENCE_TOKENS)[None, :, None]
    spike_matches = token_position == spike_position[:, :, None]
    spike_list = jnp.sum(jnp.where(spike_matches, jnp.log(spike_retained)[:, None, :], 0.0), axis=0)
    return (-decay_speed[None, :] * segment_multiplier * jaggedness + spike_list).astype(jnp.float32)


def with_spikes(values, own_key, source, target, blocks, factor):
    def block_of(position):
        return (jnp.arange(values.shape[position]) // (values.shape[position] // blocks)).reshape((-1,) + (1,) * (values.ndim - 1 - position))

    one_side = jax.random.permutation(own_key, blocks)[block_of(target)]
    other_side = (block_of(target) + blocks // 2) % blocks
    return jnp.where((block_of(source) == one_side) | (block_of(source) == other_side), factor * values, values)


def block_scale(own_key, shape, shards, least, largest):
    factor_of, own = 1.0, jax.random.fold_in(own_key, 6)
    for position, shards_of in shards:
        draws = jnp.exp(jax.random.uniform(jax.random.fold_in(own, position), (shards_of,), jnp.float32, least / len(shards), largest / len(shards)))
        factor_of = factor_of * jnp.repeat(draws, shape[position] // shards_of).reshape([-1 if axis == position else 1 for axis in range(len(shape))])
    return factor_of


def assign_block(key, own, number, rows, number_of, top, bound, slope):
    sequence = jax.random.permutation(key, number_of)
    packed, usual = portions_of(number_of, rows * top, bound, slope, True), portions_of(number_of, rows * top, bound, slope, False)
    places = jnp.arange(number_of)

    def named(lengths, offset_by):
        used = int((lengths > 0).sum())
        fixed = max(1, used // 4)
        passed = fixed + (places - fixed + offset_by * (used - fixed)) % max(1, number_of - fixed)
        return jnp.zeros((number_of,), jnp.int32).at[sequence[jnp.where(places < fixed, places, passed)]].set(jnp.asarray(lengths, jnp.int32))

    lengths = jnp.where(number % 4 == 0, named(packed, number // 4), named(usual, number - number // 4 - 1))
    mixed = jax.random.permutation(jax.random.fold_in(own, 3), number_of)
    giver, taker = mixed[0:number_of // 2 * 2:2], mixed[1:number_of // 2 * 2:2]
    room = jnp.minimum(lengths[giver] - 1, bound - lengths[taker]) // 2
    room = jnp.where((giver == sequence[0]) | (taker == sequence[0]) | (lengths[taker] == 0), 0, jnp.maximum(room, 0))
    passed = jax.random.randint(jax.random.fold_in(own, 4), (number_of // 2,), 0, 1 << 20) % (room + 1)
    lengths = lengths.at[giver].add(-passed).at[taker].add(passed)
    items = jnp.searchsorted(jnp.cumsum(lengths), jnp.arange(rows * top), side="right").astype(jnp.int32)
    listing = items.reshape(top, rows).T
    listing = listing[jax.random.permutation(jax.random.fold_in(own, 1), rows)]
    offset_by = jax.random.randint(jax.random.fold_in(own, 2), (rows, 1), 0, top)
    return jnp.take_along_axis(listing, (jnp.arange(top)[None, :] + offset_by) % top, axis=1)


def portions_of(amount, total, bound, slope, full):
    weights = [(1 << 20) // math.isqrt(grade ** slope) + 1 for grade in range(1, amount + 1)]
    largest = bound if full else min(bound, max(-(-total // amount), total * weights[0] // sum(weights)))
    least = 1 if total - largest >= amount - 1 else 0
    counts, spare = [largest] + [least] * (amount - 1), total - largest - least * (amount - 1)
    while spare > 0:
        free = [i for i in range(1, amount) if counts[i] < largest] or [i for i in range(1, amount) if counts[i] < bound]
        mass, budget = sum([weights[i] for i in free]), spare
        for i in free:
            extra = min(bound - counts[i], max(1, budget * weights[i] // mass), spare)
            counts[i] = counts[i] + extra
            spare = spare - extra
    return np.array(counts)


def centred(stream_key, extent, scale, bound, cuts=(), kind=jnp.bfloat16):
    level = block_scale(stream_key, extent, cuts, -0.22, 0.18) if cuts else 1.0
    values = jax.random.normal(stream_key, extent, jnp.float32) * scale * level
    return jnp.minimum(jnp.maximum(values, -bound), bound).astype(kind)


def bell_draw_with(stream_key, shape, scale, reach, shards, heavy, kind=jnp.bfloat16):
    result = scale * jax.random.normal(stream_key, shape, jnp.float32)
    if shards:
        result = result * block_scale(stream_key, shape, shards, -0.22, 0.18)
    return jnp.clip(with_spikes(result, jax.random.fold_in(stream_key, 3), *heavy), -reach, reach).astype(kind)


def setup_inputs(seed: int = 0) -> dict:
    keys = jax.random.split(jax.random.key(seed), 16)
    residual_mid = draw_residual_mid(jax.random.fold_in(keys[15], 71), 0)
    out_grad = bell_draw_with(keys[1], (SEQUENCE_TOKENS, D), 1.0, 6.0, ((0, 4),), (0, 1, 4, 2.0))
    norm_gain = jnp.clip(1.0 + 0.18 * jax.random.normal(keys[2], (D,), jnp.float32), 0.1, 1.9)
    expert_ids_keys = jax.random.split(jax.random.fold_in(keys[3], 1), SEQUENCE_TOKENS // TOK_DEV)
    expert_ids_turns = jax.random.permutation(jax.random.fold_in(keys[3], 3), SEQUENCE_TOKENS // TOK_DEV)
    expert_ids = jax.vmap(lambda own, number: assign_block(jax.random.fold_in(keys[3], 2), own, number, TOK_DEV, EXPERTS, TOP, CAP, 2))(expert_ids_keys, expert_ids_turns).reshape((SEQUENCE_TOKENS, TOP))
    expert_weights = jnp.clip(0.1 + 0.9 * jax.random.uniform(keys[4], (SEQUENCE_TOKENS, TOP), jnp.float32) ** block_scale(keys[4], (SEQUENCE_TOKENS, TOP), ((0, 4),), -0.2, 0.2), 0.1, 1.0)
    gate_proj = centred(keys[5], (EXPERTS, D, FF), (D // 9) ** -0.5, 0.25, ((0, 4), (2, 8)))
    up_proj = centred(keys[6], (EXPERTS, D, FF), (D // 9) ** -0.5, 0.25, ((0, 4), (2, 8)))
    down_proj = centred(keys[7], (EXPERTS, FF, D), FF ** -0.5, 0.125, ((0, 4), (1, 8)))
    out_proj = centred(keys[8], (RW, D), RW ** -0.5, 0.09375, ((0, 8),))
    query_rows = centred(keys[9], (SEQUENCE_TOKENS, RW), 1.0, 6.0, ((0, 4), (1, 8)))
    key_rows = centred(keys[10], (SEQUENCE_TOKENS, RW), 1.0, 6.0, ((0, 4), (1, 8)))
    value_rows = centred(keys[11], (SEQUENCE_TOKENS, RW), 1.0, 6.0, ((0, 4), (1, 8)))
    retention_out = centred(keys[12], (SEQUENCE_TOKENS, RW), 1.0, 6.0, ((0, 4), (1, 8)))
    log_decay = draw_log_decay(jax.random.fold_in(keys[15], 71), 0)
    entry_state = centred(keys[14], (SEGS, RETENTION_HEADS, DK, DK), 4.0, 24.0, ((0, 4), (1, 8)), jnp.float32)
    return dict(residual_mid=residual_mid, out_grad=out_grad, norm_gain=norm_gain, expert_ids=expert_ids, expert_weights=expert_weights, gate_proj=gate_proj, up_proj=up_proj, down_proj=down_proj, out_proj=out_proj, query_rows=query_rows, key_rows=key_rows, value_rows=value_rows, retention_out=retention_out, log_decay=log_decay, entry_state=entry_state)


CLAMP_LIMIT = 7.0
GATE_ALPHA = 1.702
NORM_EPSILON = 1e-05

def activate(gate_pre, up_pre):
    gate_clamped = jnp.minimum(gate_pre, CLAMP_LIMIT)
    up_clamped = jnp.clip(up_pre, -CLAMP_LIMIT, CLAMP_LIMIT)
    return (up_clamped + 1.0) * gate_clamped * jax.nn.sigmoid(GATE_ALPHA * gate_clamped)

def reference(residual_mid, out_grad, norm_gain, expert_ids, expert_weights, gate_proj, up_proj, down_proj, out_proj, query_rows, key_rows, value_rows, retention_out, log_decay, entry_state):
    top_count = expert_ids.shape[1]
    width = residual_mid.shape[1]
    pair_count = SEQUENCE_TOKENS * top_count
    mid_rows = residual_mid.astype(jnp.float32)
    inverse = lax.rsqrt(lax.optimization_barrier(jnp.mean(mid_rows * mid_rows, axis=1, keepdims=True)) + NORM_EPSILON)
    scaled = mid_rows * inverse
    normed = (scaled * norm_gain).astype(jnp.bfloat16)
    flat_ids = expert_ids.reshape(SEGS, TOK_DEV * top_count).astype(jnp.int32)
    chosen = (flat_ids[:, :, None] == jnp.arange(EXPERTS, dtype=jnp.int32)[None, None, :]).astype(jnp.int32)
    placed = lax.optimization_barrier(jnp.sum((jnp.cumsum(chosen, axis=1) - chosen) * chosen, axis=2)).astype(jnp.int32)
    segment = jnp.broadcast_to(jnp.arange(SEGS, dtype=jnp.int32)[:, None], flat_ids.shape)
    pair_index = jnp.arange(pair_count, dtype=jnp.int32).reshape(SEGS, TOK_DEV * top_count)
    slot_pair = jnp.full((EXPERTS, SEGS, CAP), pair_count, jnp.int32).at[flat_ids, segment, placed].set(pair_index)
    blank = jnp.zeros((1, width), jnp.bfloat16)
    token_table = jnp.concatenate([jnp.repeat(normed, top_count, axis=0), blank], axis=0)
    pair_grads = (expert_weights[:, :, None] * out_grad[:, None, :]).astype(jnp.bfloat16).reshape(pair_count, width)
    grad_table = jnp.concatenate([pair_grads, blank], axis=0)
    group_width = FF // N_TP

    def one_expert(operands):
        slot_rows, gate_weight, up_weight, down_weight = operands
        slot_index = slot_rows.reshape(-1)
        rows_in = token_table[slot_index]
        rows_grad = grad_table[slot_index]
        gate_pre = jnp.dot(rows_in, gate_weight, preferred_element_type=jnp.float32)
        up_pre = jnp.dot(rows_in, up_weight, preferred_element_type=jnp.float32)
        hidden, pullback = jax.vjp(activate, gate_pre, up_pre)
        down_part = jnp.dot(hidden.astype(jnp.bfloat16).T, rows_grad, preferred_element_type=jnp.float32).astype(jnp.bfloat16)
        hidden_grad = jnp.dot(rows_grad, down_weight.T, preferred_element_type=jnp.float32)
        gate_back, up_back = pullback(hidden_grad)
        gate_back = gate_back.astype(jnp.bfloat16)
        up_back = up_back.astype(jnp.bfloat16)
        gate_part = jnp.dot(rows_in.T, gate_back, preferred_element_type=jnp.float32).astype(jnp.bfloat16)
        up_part = jnp.dot(rows_in.T, up_back, preferred_element_type=jnp.float32).astype(jnp.bfloat16)
        row_total = rows_in.shape[0]
        parts = jnp.einsum('rjf,djf->jrd', gate_back.astype(jnp.float32).reshape(row_total, N_TP, group_width), gate_weight.astype(jnp.float32).reshape(width, N_TP, group_width))
        parts = parts + jnp.einsum('rjf,djf->jrd', up_back.astype(jnp.float32).reshape(row_total, N_TP, group_width), up_weight.astype(jnp.float32).reshape(width, N_TP, group_width))
        rounded = lax.optimization_barrier(parts.astype(jnp.bfloat16))
        summed = lax.optimization_barrier(jnp.sum(rounded.astype(jnp.float32), axis=0)).astype(jnp.bfloat16)
        return (gate_part, up_part, down_part, summed)
    gate_grad, up_grad, down_grad, returned = lax.map(one_expert, (slot_pair, gate_proj, up_proj, down_proj))
    picked = returned[flat_ids, segment * CAP + placed]
    mixed_grad = lax.optimization_barrier(jnp.sum(picked.reshape(SEQUENCE_TOKENS, top_count, width).astype(jnp.float32), axis=1))
    weighted = norm_gain * mixed_grad
    inner = lax.optimization_barrier(jnp.mean(scaled * weighted, axis=1, keepdims=True))
    resid_grad = (out_grad.astype(jnp.float32) + inverse * (weighted - scaled * inner)).astype(jnp.bfloat16)
    proj_grad = jnp.dot(resid_grad.T, retention_out, preferred_element_type=jnp.float32)
    head_grad = jnp.dot(resid_grad, out_proj.T, preferred_element_type=jnp.float32)
    heads = log_decay.shape[1]
    highest = lax.Precision.HIGHEST

    def split_heads(rows):
        return rows.astype(jnp.float32).reshape(SEGS, TOK_DEV, heads, -1).transpose(0, 2, 1, 3)
    queries = split_heads(query_rows)
    key_heads = split_heads(key_rows)
    value_heads = split_heads(value_rows)
    grad_heads = split_heads(head_grad)
    key_scale = queries.shape[3] ** (-0.5)
    running = jnp.cumsum(log_decay.reshape(SEGS, TOK_DEV, heads), axis=1).transpose(0, 2, 1)
    from_start = jnp.exp(running)
    to_end = jnp.exp(running[:, :, -1:] - running)
    token_position = jnp.arange(TOK_DEV, dtype=jnp.int32)
    causal = (token_position[:, None] >= token_position[None, :])[None, None]
    spread = jnp.where(causal, running[:, :, :, None] - running[:, :, None, :], 0.0)
    weights = jnp.where(causal, jnp.exp(spread), 0.0)
    local_state = jnp.einsum('ght,ghtk,ghte->ghke', from_start, queries, grad_heads, precision=highest)
    carry_rate = from_start[:, :, -1]

    def backward_step(carried, inputs):
        rate_now, local_now = inputs
        return (local_now + rate_now[:, None, None] * carried, carried)
    later_state = lax.scan(backward_step, jnp.zeros(local_state.shape[1:], jnp.float32), (carry_rate, local_state), reverse=True)[1]
    grad_scores = jnp.einsum('ghte,ghse->ghts', grad_heads, value_heads, precision=highest) * weights
    key_scores = jnp.einsum('ghtk,ghsk->ghts', queries, key_heads, precision=highest) * weights
    query_grad = key_scale * (jnp.einsum('ghts,ghsk->ghtk', grad_scores, key_heads, precision=highest) + from_start[..., None] * jnp.einsum('ghte,ghke->ghtk', grad_heads, entry_state, precision=highest))
    key_grad = key_scale * (jnp.einsum('ghts,ghtk->ghsk', grad_scores, queries, precision=highest) + to_end[..., None] * jnp.einsum('ghse,ghke->ghsk', value_heads, later_state, precision=highest))
    value_grad = key_scale * (jnp.einsum('ghts,ghte->ghse', key_scores, grad_heads, precision=highest) + to_end[..., None] * jnp.einsum('ghsk,ghke->ghse', key_heads, later_state, precision=highest))

    def merge_heads(heads_rows):
        return heads_rows.transpose(0, 2, 1, 3).reshape(SEQUENCE_TOKENS, -1).astype(jnp.bfloat16)
    return (gate_grad, up_grad, down_grad, proj_grad, merge_heads(query_grad), merge_heads(key_grad), merge_heads(value_grad))
```

```python
import jax
import jax.numpy as jnp
from jax import lax
from jax.sharding import Mesh, PartitionSpec as P

CLAMP_LIMIT = 7.0
GATE_ALPHA = 1.702
NORM_EPSILON = 1e-05
CORES = 2
SWAP = [(0, 1), (1, 0)]


def activate(gate_pre, up_pre):
    gate_clamped = jnp.minimum(gate_pre, CLAMP_LIMIT)
    up_clamped = jnp.clip(up_pre, -CLAMP_LIMIT, CLAMP_LIMIT)
    return (up_clamped + 1.0) * gate_clamped * jax.nn.sigmoid(GATE_ALPHA * gate_clamped)


def contract_rows(left, right):
    return lax.dot_general(
        left, right, (((0,), (0,)), ((), ())), preferred_element_type=jnp.float32
    )


def contract_cols(left, right):
    return lax.dot_general(
        left, right, (((1,), (1,)), ((), ())), preferred_element_type=jnp.float32
    )


def dots(spec, left, right):
    return jnp.einsum(
        spec,
        left.astype(jnp.bfloat16),
        right.astype(jnp.bfloat16),
        preferred_element_type=jnp.float32,
    )


def local(
    residual_mid,
    out_grad,
    norm_gain,
    expert_ids,
    expert_weights,
    gate_proj,
    up_proj,
    down_proj,
    out_proj,
    query_rows,
    key_rows,
    value_rows,
    retention_out,
    log_decay,
    entry_state,
):
    token_count, width = residual_mid.shape
    segs = lax.axis_size("sp")
    depth = lax.axis_size("z")
    seg = lax.axis_index("sp")
    core = lax.axis_index("core")
    half = token_count // CORES
    share = half // depth

    def rows_of(array, start, count):
        return lax.dynamic_slice_in_dim(array, start, count, axis=0)

    def normalize(rows):
        wide = rows.astype(jnp.float32)
        inverse = lax.rsqrt(jnp.mean(wide * wide, axis=1, keepdims=True) + NORM_EPSILON)
        return wide * inverse, inverse

    grad_own = lax.all_gather(rows_of(out_grad, core * half, half), "sp").reshape(-1, width)
    normed_half = (normalize(rows_of(residual_mid, core * half, half))[0] * norm_gain).astype(
        jnp.bfloat16
    )
    normed_own = lax.all_gather(normed_half, "sp").reshape(-1, width)
    grad_other = lax.ppermute(grad_own, "core", SWAP)
    normed_other = lax.ppermute(normed_own, "core", SWAP)

    experts = jnp.arange(segs, dtype=jnp.int32)
    route = jnp.sum(
        jnp.where(expert_ids.T[None] == experts[:, None, None], expert_weights.T[None], 0.0), axis=1
    )
    heads_here = log_decay.shape[1]
    small = jnp.concatenate([route.reshape(-1), jnp.sum(log_decay, axis=0)])
    smalls = lax.all_gather(small, "sp")
    routes = smalls[:, : segs * token_count].reshape(segs, segs, token_count)
    seg_decay = smalls[:, segs * token_count :]
    here = lax.dynamic_index_in_dim(routes, seg, axis=1, keepdims=False)
    here = here.reshape(segs, CORES, half)
    weight_own = lax.dynamic_index_in_dim(here, core, axis=1, keepdims=False).reshape(-1, 1)
    weight_other = lax.dynamic_index_in_dim(here, 1 - core, axis=1, keepdims=False).reshape(-1, 1)

    gate_weight = gate_proj[0]
    up_weight = up_proj[0]
    down_weight = down_proj[0]

    def expert(rows_in, rows_out, weight):
        rows_grad = (weight * rows_out.astype(jnp.float32)).astype(jnp.bfloat16)
        gate_pre = jnp.dot(rows_in, gate_weight, preferred_element_type=jnp.float32)
        up_pre = jnp.dot(rows_in, up_weight, preferred_element_type=jnp.float32)
        hidden, pullback = jax.vjp(activate, gate_pre, up_pre)
        gate_back, up_back = pullback(contract_cols(rows_grad, down_weight))
        gate_back = gate_back.astype(jnp.bfloat16)
        up_back = up_back.astype(jnp.bfloat16)
        part = contract_cols(gate_back, gate_weight) + contract_cols(up_back, up_weight)
        return part, rows_grad, hidden.astype(jnp.bfloat16), gate_back, up_back

    part_own, cot_own, hidden_own, gate_back_own, up_back_own = expert(
        normed_own, grad_own, weight_own
    )
    part_other, cot_other, hidden_other, gate_back_other, up_back_other = expert(
        normed_other, grad_other, weight_other
    )
    part_got = lax.ppermute(part_other.astype(jnp.bfloat16), "core", SWAP)
    part_pair = (part_own + part_got.astype(jnp.float32)).astype(jnp.bfloat16)
    part_seg = lax.psum_scatter(
        part_pair.reshape(segs, half, width), "sp", scatter_dimension=0, tiled=False
    )
    mixed_grad = lax.psum_scatter(
        part_seg.reshape(depth, share, width), "z", scatter_dimension=0, tiled=False
    ).astype(jnp.float32)

    down_grad = (contract_rows(hidden_own, cot_own) + contract_rows(hidden_other, cot_other)).astype(
        jnp.bfloat16
    )[None]
    gate_grad = (
        contract_rows(normed_own, gate_back_own) + contract_rows(normed_other, gate_back_other)
    ).astype(jnp.bfloat16)[None]
    up_grad = (
        contract_rows(normed_own, up_back_own) + contract_rows(normed_other, up_back_other)
    ).astype(jnp.bfloat16)[None]

    start = core * half + lax.axis_index("z") * share
    scaled, inverse = normalize(rows_of(residual_mid, start, share))
    weighted = norm_gain * mixed_grad
    inner = jnp.mean(scaled * weighted, axis=1, keepdims=True)
    resid_part = (
        rows_of(out_grad, start, share).astype(jnp.float32)
        + inverse * (weighted - scaled * inner)
    ).astype(jnp.bfloat16)
    resid_grad = lax.all_gather(resid_part, ("core", "z"), axis=0, tiled=False).reshape(
        token_count, width
    )
    columns = lax.all_to_all(
        resid_part.reshape(share, segs, width // segs).transpose(1, 0, 2),
        "sp",
        split_axis=0,
        concat_axis=0,
        tiled=True,
    )
    columns = lax.all_gather(columns, ("core", "z"), axis=0, tiled=False).reshape(
        segs * token_count, -1
    )
    outs = lax.all_gather(retention_out, "sp")
    outs = outs.reshape(segs, CORES * depth, share, -1).transpose(1, 0, 2, 3)
    outs = outs.reshape(segs * token_count, -1)
    proj_grad = contract_rows(columns, outs)

    head_grad = contract_cols(resid_grad, out_proj).astype(jnp.bfloat16)

    def split_heads(rows):
        return rows.reshape(token_count, heads_here, -1).transpose(1, 0, 2)

    queries = split_heads(query_rows)
    key_heads = split_heads(key_rows)
    value_heads = split_heads(value_rows)
    grad_heads = split_heads(head_grad)
    key_scale = queries.shape[2] ** (-0.5)
    running = jnp.cumsum(log_decay, axis=0).T
    from_start = jnp.exp(running)
    to_end = jnp.exp(running[:, -1:] - running)
    position = jnp.arange(token_count, dtype=jnp.int32)
    causal = (position[:, None] >= position[None, :])[None]
    spread = jnp.where(causal, running[:, :, None] - running[:, None, :], 0.0)
    weights = jnp.where(causal, jnp.exp(spread), 0.0)
    local_state = dots("htk,hte->hke", from_start[:, :, None] * queries, grad_heads)
    states = lax.all_gather(local_state.astype(jnp.bfloat16), "sp")
    order = jnp.arange(segs, dtype=jnp.int32)
    between = (order[None, :] > seg) & (order[None, :] < order[:, None])
    passed = jnp.exp(jnp.sum(jnp.where(between[:, :, None], seg_decay[None], 0.0), axis=1))
    passed = jnp.where(order[:, None] > seg, passed, 0.0)
    later_state = jnp.sum(passed[:, :, None, None] * states.astype(jnp.float32), axis=0)
    entry = entry_state[0]
    grad_scores = dots("hte,hse->hts", grad_heads, value_heads) * weights
    key_scores = dots("htk,hsk->hts", queries, key_heads) * weights
    query_grad = key_scale * (
        dots("hts,hsk->htk", grad_scores, key_heads)
        + from_start[:, :, None] * dots("hte,hke->htk", grad_heads, entry)
    )
    key_grad = key_scale * (
        dots("hts,htk->hsk", grad_scores, queries)
        + to_end[:, :, None] * dots("hse,hke->hsk", value_heads, later_state)
    )
    value_grad = key_scale * (
        dots("hts,hte->hse", key_scores, grad_heads)
        + to_end[:, :, None] * dots("hsk,hke->hse", key_heads, later_state)
    )

    def merge_heads(heads_rows):
        return heads_rows.transpose(1, 0, 2).reshape(token_count, -1).astype(jnp.bfloat16)

    return (
        gate_grad,
        up_grad,
        down_grad,
        proj_grad,
        merge_heads(query_grad),
        merge_heads(key_grad),
        merge_heads(value_grad),
    )


def solution(mesh):
    segs, split = mesh.shape["sp"], mesh.shape["tp"]
    fine = Mesh(mesh.devices.reshape(segs, split // CORES, CORES), ("sp", "z", "core"))
    tp = ("z", "core")
    placed = (
        P("sp", None),
        P("sp", None),
        P(),
        P("sp", None),
        P("sp", None),
        P("sp", None, tp),
        P("sp", None, tp),
        P("sp", tp, None),
        P(tp, None),
        P("sp", tp),
        P("sp", tp),
        P("sp", tp),
        P("sp", tp),
        P("sp", tp),
        P("sp", tp, None, None),
    )
    return jax.shard_map(
        local,
        mesh=fine,
        in_specs=placed,
        out_specs=(
            P("sp", None, tp),
            P("sp", None, tp),
            P("sp", tp, None),
            P("sp", tp),
            P("sp", tp),
            P("sp", tp),
            P("sp", tp),
        ),
        check_vma=False,
    )
```
